32 devices in a mesh: ep: 16 (over z, y, core), tp: 2 (over x).
Axes of the slice: x: 2, y: 2, z: 4, core: 2. Of those that a mesh axis runs over, the one named last changes fastest.
Arguments:
- tokens: bfloat16 [128, 1024], P(('ep', 'tp')), may hold values from -6 to 6
- lengths: int32 [128], P(('ep', 'tp')), may hold values from 256 to 1024, as said below
- cache_latent: bfloat16 [128, 1024, 256], P(('ep', 'tp')), may hold values from -160 to 160
- cache_rope: bfloat16 [128, 32, 1024], P(('ep', 'tp')), may hold values from -6 to 6
- attn_gain: float32 [1024], replicated, may hold values from 0.1 to 1.9
- latent_gain: float32 [256], replicated, may hold values from 0.1 to 1.9
- post_gain: float32 [1024], replicated, may hold values from 0.1 to 1.9
- ffn_gain: float32 [1024], replicated, may hold values from 0.1 to 1.9
- out_gain: float32 [1024], replicated, may hold values from 0.1 to 1.9
- w_latent: bfloat16 [1024, 256], P(None, 'tp'), may hold values from -0.1875 to 0.1875
- w_rope_key: bfloat16 [1024, 32], replicated, may hold values from -0.1875 to 0.1875
- w_query: bfloat16 [1024, 768], P(None, 'tp'), may hold values from -0.1875 to 0.1875
- w_absorb_key: bfloat16 [8, 64, 256], P('tp'), may hold values from -0.75 to 0.75
- w_absorb_value: bfloat16 [8, 256, 64], P('tp'), may hold values from -0.375 to 0.375
- w_out: bfloat16 [512, 1024], P('tp'), may hold values from -0.25 to 0.25
- routes: int32 [128, 6], P(('ep', 'tp')), may hold values from 0 to 15, all different within a row; in each aligned block of 8 rows (0 to 7, 8 to 15, ...) at most 5 rows name the same one
- route_weights: float32 [128, 6], P(('ep', 'tp')), may hold values from 0.2 to 1
- w_exp_gate: bfloat16 [16, 1024, 256], P('ep'), may hold values from -0.1875 to 0.1875
- w_exp_up: bfloat16 [16, 1024, 256], P('ep'), may hold values from -0.1875 to 0.1875
- w_exp_down: bfloat16 [16, 256, 1024], P('ep'), may hold values from -0.375 to 0.375
- w_dense_gate: bfloat16 [4096, 1024], P('ep'), may hold values from -0.1875 to 0.1875
- w_dense_up: bfloat16 [4096, 1024], P('ep'), may hold values from -0.1875 to 0.1875
- w_dense_down: bfloat16 [4096, 1024], P('ep'), may hold values from -0.09375 to 0.09375
- dense_gate_vector: float32 [1024], replicated, may hold values from -0.1875 to 0.1875
Outputs:
- output: bfloat16 [128, 1024], P(('ep', 'tp'))
- new_latent: bfloat16 [128, 256], P(('ep', 'tp'))
- new_rope_key: bfloat16 [128, 32], P(('ep', 'tp'))
The draws below stay inside these ranges and needn't reach their ends.
Inputs may be any that keep to these rules, and one draw needn't show every extreme that they name: `routes`: in each aligned block of 8 rows no expert is named by more than 5 rows; each row names 6 different experts. `lengths`: some sequence holds exactly 1024 cached positions.
All inputs are finite; a program needn't handle non-finite values.
Results may differ from the reference program's by a relative error of at most 0.015.
Values may be sent and summed in bfloat16 or wider, within the bound.
A program may use at most 64 MiB of HBM per device.

```python
import math
import jax
import jax.numpy as jnp
import numpy as np
from jax import lax

D = 1024
HEADS = 8
NOPE = 64
ROPE = 32
V_HEAD = 64
KV_RANK = 256
EXPERT_FF = 256
SH_FF = 4096
TOPK = 6
CACHE_LEN = 1024
SEQ_GRP = 8
BATCH = 128
EXPERTS = 16
CAP = 5
N_EP = 16
N_TP = 2


def draw_lengths(key, part):
    first_key, second_key = jax.random.split(key)
    drawn = jax.random.randint(first_key, (BATCH,), CACHE_LEN // 4, CACHE_LEN + 1)
    chosen = jax.random.randint(second_key, (), 0, BATCH)
    return jnp.where(jnp.arange(BATCH) == chosen, CACHE_LEN, drawn).astype(jnp.int32)


def draw_cache_latent(key, part):
    keys = jax.random.split(key, 1)
    base = jnp.clip(jax.random.normal(keys[0], (BATCH, CACHE_LEN, KV_RANK), jnp.float32), -4.0, 4.0)
    return base.astype(jnp.bfloat16)


def block_levels(rng, shape, cuts, smallest, largest):
    def one(dim, blocks):
        draws = jax.random.uniform(jax.random.fold_in(jax.random.fold_in(rng, 6), dim), (blocks,), jnp.float32, smallest / len(cuts), largest / len(cuts))
        return jnp.repeat(jnp.exp(draws), shape[dim] // blocks).reshape((-1,) + (1,) * (len(shape) - dim - 1))

    level = one(*cuts[0])
    for cut in cuts[1:]:
        level = level * one(*cut)
    return level


def deal_out(key, own, number, rows, number_of, top, bound, skew):
    ranking = jax.random.permutation(key, number_of)
    packed, ordinary = load_shares(number_of, rows * top, bound, skew, True), load_shares(number_of, rows * top, bound, skew, False)
    places = jnp.arange(number_of)

    def named(sizes, rotation):
        used = int((sizes > 0).sum())
        fixed = max(1, used // 4)
        shifted = fixed + (places - fixed + rotation * (used - fixed)) % max(1, number_of - fixed)
        return jnp.zeros((number_of,), jnp.int32).at[ranking[jnp.where(places < fixed, places, shifted)]].set(jnp.asarray(sizes, jnp.int32))

    sizes = jnp.where(number % 4 == 0, named(packed, number // 4), named(ordinary, number - number // 4 - 1))
    mixed = jax.random.permutation(jax.random.fold_in(own, 3), number_of)
    source_of, sink = mixed[0:number_of // 2 * 2:2], mixed[1:number_of // 2 * 2:2]
    margin = jnp.minimum(sizes[source_of] - 1, bound - sizes[sink]) // 2
    margin = jnp.where((source_of == ranking[0]) | (sink == ranking[0]) | (sizes[sink] == 0), 0, jnp.maximum(margin, 0))
    shifted = jax.random.randint(jax.random.fold_in(own, 4), (number_of // 2,), 0, 1 << 20) % (margin + 1)
    sizes = sizes.at[source_of].add(-shifted).at[sink].add(shifted)
    items = jnp.searchsorted(jnp.cumsum(sizes), jnp.arange(rows * top), side="right").astype(jnp.int32)
    grid = items.reshape(top, rows).T
    grid = grid[jax.random.permutation(jax.random.fold_in(own, 1), rows)]
    rotation = jax.random.randint(jax.random.fold_in(own, 2), (rows, 1), 0, top)
    return jnp.take_along_axis(grid, (jnp.arange(top)[None, :] + rotation) % top, axis=1)


def load_shares(number_of, total, bound, lean, full):
    weights = [(1 << 20) // math.isqrt(standing ** lean) + 1 for standing in range(1, number_of + 1)]
    largest = bound if full else min(bound, max(-(-total // number_of), total * weights[0] // sum(weights)))
    least = 1 if total - largest >= number_of - 1 else 0
    holding, spare = [largest] + [least] * (number_of - 1), total - largest - least * (number_of - 1)
    while spare > 0:
        candidates = [i for i in range(1, number_of) if holding[i] < largest] or [i for i in range(1, number_of) if holding[i] < bound]
        whole, budget = sum([weights[i] for i in candidates]), spare
        for i in candidates:
            extra = min(bound - holding[i], max(1, budget * weights[i] // whole), spare)
            holding[i] = holding[i] + extra
            spare = spare - extra
    return np.array(holding)


def gaussian(stream_key, extent, scale, limit, cuts=(), kind=jnp.bfloat16):
    values = jax.random.normal(stream_key, extent, jnp.float32) * scale
    if len(cuts) > 0:
        values = block_levels(stream_key, extent, cuts, -0.22, 0.18) * values
    return jnp.clip(values, min=-limit, max=limit).astype(kind)


def setup_inputs(seed: int = 0) -> dict:
    arg_keys = jax.random.split(jax.random.key(seed), 25)
    tokens = gaussian(arg_keys[0], (BATCH, D), 1.0, 6.0, ((0, 32),))
    lengths = draw_lengths(jax.random.fold_in(arg_keys[24], 71), 0)
    cache_latent = draw_cache_latent(jax.random.fold_in(arg_keys[24], 71), 0)
    cache_rope = gaussian(arg_keys[3], (BATCH, ROPE, CACHE_LEN), 1.0, 6.0, ((0, 32),))
    attn_gain = jnp.clip(1.0 + 0.18 * jax.random.normal(arg_keys[4], (D,), jnp.float32), 0.1, 1.9)
    latent_gain = jnp.clip(1.0 + 0.18 * jax.random.normal(arg_keys[5], (KV_RANK,), jnp.float32), 0.1, 1.9)
    post_gain = jnp.clip(1.0 + 0.18 * jax.random.normal(arg_keys[6], (D,), jnp.float32), 0.1, 1.9)
    ffn_gain = jnp.clip(1.0 + 0.18 * jax.random.normal(arg_keys[7], (D,), jnp.float32), 0.1, 1.9)
    out_gain = jnp.clip(1.0 + 0.18 * jax.random.normal(arg_keys[8], (D,), jnp.float32), 0.1, 1.9)
    w_latent = gaussian(arg_keys[9], (D, KV_RANK), D ** -0.5, 0.1875, ((1, 2),))
    w_rope_key = gaussian(arg_keys[10], (D, ROPE), D ** -0.5, 0.1875)
    w_query = gaussian(arg_keys[11], (D, HEADS * (NOPE + ROPE)), D ** -0.5, 0.1875, ((1, 2),))
    w_absorb_key = gaussian(arg_keys[12], (HEADS, NOPE, KV_RANK), NOPE ** -0.5, 0.75, ((0, 2),))
    w_absorb_value = gaussian(arg_keys[13], (HEADS, KV_RANK, V_HEAD), KV_RANK ** -0.5, 0.375, ((0, 2),))
    w_out = gaussian(arg_keys[14], (HEADS * V_HEAD, D), (HEADS * V_HEAD) ** -0.5, 0.25, ((0, 2),))
    routes_keys = jax.random.split(jax.random.fold_in(arg_keys[15], 1), BATCH // SEQ_GRP)
    routes_turns = jax.random.permutation(jax.random.fold_in(arg_keys[15], 3), BATCH // SEQ_GRP)
    routes = jax.vmap(lambda own, number: deal_out(jax.random.fold_in(arg_keys[15], 2), own, number, SEQ_GRP, EXPERTS, TOPK, CAP, 2))(routes_keys, routes_turns).reshape((BATCH, TOPK))
    route_weights = jnp.clip(0.2 + 0.8 * jax.random.uniform(arg_keys[16], (BATCH, TOPK), jnp.float32) ** block_levels(arg_keys[16], (BATCH, TOPK), ((0, 32),), -0.2, 0.2), 0.2, 1.0)
    w_exp_gate = gaussian(arg_keys[17], (EXPERTS, D, EXPERT_FF), D ** -0.5, 0.1875, ((0, 16),))
    w_exp_up = gaussian(arg_keys[18], (EXPERTS, D, EXPERT_FF), D ** -0.5, 0.1875, ((0, 16),))
    w_exp_down = gaussian(arg_keys[19], (EXPERTS, EXPERT_FF, D), EXPERT_FF ** -0.5, 0.375, ((0, 16),))
    w_dense_gate = gaussian(arg_keys[20], (SH_FF, D), D ** -0.5, 0.1875, ((0, 16),))
    w_dense_up = gaussian(arg_keys[21], (SH_FF, D), D ** -0.5, 0.1875, ((0, 16),))
    w_dense_down = gaussian(arg_keys[22], (SH_FF, D), SH_FF ** -0.5, 0.09375, ((0, 16),))
    dense_gate_vector = gaussian(arg_keys[23], (D,), D ** -0.5, 0.1875, (), jnp.float32)
    return {"tokens": tokens, "lengths": lengths, "cache_latent": cache_latent, "cache_rope": cache_rope, "attn_gain": attn_gain, "latent_gain": latent_gain, "post_gain": post_gain, "ffn_gain": ffn_gain, "out_gain": out_gain, "w_latent": w_latent, "w_rope_key": w_rope_key, "w_query": w_query, "w_absorb_key": w_absorb_key, "w_absorb_value": w_absorb_value, "w_out": w_out, "routes": routes, "route_weights": route_weights, "w_exp_gate": w_exp_gate, "w_exp_up": w_exp_up, "w_exp_down": w_exp_down, "w_dense_gate": w_dense_gate, "w_dense_up": w_dense_up, "w_dense_down": w_dense_down, "dense_gate_vector": dense_gate_vector}


epsilon = 1e-06
rope_base = 10000.0
negative = -1e+30

def normalize(values, gain_vec):
    values = values.astype(jnp.float32)
    return values * lax.rsqrt(lax.optimization_barrier(jnp.mean(values * values, axis=-1, keepdims=True)) + epsilon) * gain_vec

def rotate(values, positions):
    half_width = values.shape[-1] // 2
    inverse = rope_base ** (-jnp.arange(half_width, dtype=jnp.float32) / half_width)
    angles = positions.astype(jnp.float32)[..., None] * inverse
    cosine = jnp.cos(angles)
    sine_part = jnp.sin(angles)
    first_half = values[..., :half_width]
    second = values[..., half_width:]
    return jnp.concatenate([first_half * cosine - second * sine_part, first_half * sine_part + second * cosine], axis=-1)

def attend(operands):
    q_latent, q_rope, cache_lat, cache_rot, new_lat, new_rot, seq_lengths = operands
    scaling = (NOPE + ROPE) ** (-0.5)
    scores = jnp.einsum('shc,slc->shl', q_latent.astype(jnp.float32), cache_lat.astype(jnp.float32))
    scores = scores + jnp.einsum('shr,srl->shl', q_rope.astype(jnp.float32), cache_rot.astype(jnp.float32))
    scores = scores * scaling
    own_score = lax.optimization_barrier(jnp.sum(q_latent.astype(jnp.float32) * new_lat.astype(jnp.float32)[:, None, :], axis=-1))
    own_score = (own_score + lax.optimization_barrier(jnp.sum(q_rope.astype(jnp.float32) * new_rot.astype(jnp.float32)[:, None, :], axis=-1))) * scaling
    visible = jnp.arange(cache_lat.shape[1], dtype=jnp.int32)[None, None, :] < seq_lengths[:, None, None]
    scores = jnp.where(visible, scores, negative)
    row_max = jnp.maximum(lax.optimization_barrier(jnp.max(scores, axis=-1)), own_score)
    weights = jnp.exp(scores - row_max[..., None])
    own_weight = jnp.exp(own_score - row_max)
    totals = lax.optimization_barrier(jnp.sum(weights, axis=-1)) + own_weight
    probabilities = (weights / totals[..., None]).astype(jnp.bfloat16)
    own_prob = (own_weight / totals).astype(jnp.bfloat16)
    mixed = jnp.einsum('shl,slc->shc', probabilities.astype(jnp.float32), cache_lat.astype(jnp.float32))
    mixed = mixed + own_prob.astype(jnp.float32)[..., None] * new_lat.astype(jnp.float32)[:, None, :]
    return mixed.astype(jnp.bfloat16)

def reference(tokens, lengths, cache_latent, cache_rope, attn_gain, latent_gain, post_gain, ffn_gain, out_gain, w_latent, w_rope_key, w_query, w_absorb_key, w_absorb_value, w_out, routes, route_weights, w_exp_gate, w_exp_up, w_exp_down, w_dense_gate, w_dense_up, w_dense_down, dense_gate_vector):
    hidden = normalize(tokens, attn_gain).astype(jnp.bfloat16)
    new_latent = normalize(jnp.dot(hidden, w_latent, preferred_element_type=jnp.float32), latent_gain).astype(jnp.bfloat16)
    new_rope_key = rotate(jnp.dot(hidden, w_rope_key, preferred_element_type=jnp.float32), lengths).astype(jnp.bfloat16)
    queries = jnp.dot(hidden, w_query, preferred_element_type=jnp.float32).astype(jnp.bfloat16)
    queries = queries.reshape(BATCH, HEADS, NOPE + ROPE)
    query_rope = rotate(queries[..., NOPE:].astype(jnp.float32), lengths[:, None]).astype(jnp.bfloat16)
    query_latent = jnp.einsum('shn,hnc->shc', queries[..., :NOPE].astype(jnp.float32), w_absorb_key.astype(jnp.float32)).astype(jnp.bfloat16)

    def grouped(array):
        return array.reshape((N_EP, SEQ_GRP) + array.shape[1:])
    attended = lax.map(attend, (grouped(query_latent), grouped(query_rope), grouped(cache_latent), grouped(cache_rope), grouped(new_latent), grouped(new_rope_key), grouped(lengths)))
    attended = attended.reshape(BATCH, HEADS, KV_RANK)
    head_out = jnp.einsum('shc,hcv->shv', attended.astype(jnp.float32), w_absorb_value.astype(jnp.float32)).astype(jnp.bfloat16)
    per_group = HEADS // N_TP
    pieces = jnp.einsum('sgk,gkd->sgd', head_out.reshape(BATCH, N_TP, per_group * V_HEAD).astype(jnp.float32), w_out.reshape(N_TP, per_group * V_HEAD, D).astype(jnp.float32))
    pieces = lax.optimization_barrier(pieces.astype(jnp.bfloat16))
    mixed = lax.optimization_barrier(jnp.sum(pieces.astype(jnp.float32), axis=1))
    residual = (tokens.astype(jnp.float32) + normalize(mixed, post_gain)).astype(jnp.bfloat16)
    ffn_in = normalize(residual, ffn_gain).astype(jnp.bfloat16)
    flattened = routes.reshape(N_EP, SEQ_GRP * TOPK)
    onehot = (flattened[..., None] == jnp.arange(EXPERTS, dtype=jnp.int32)).astype(jnp.int32)
    order_rank = lax.optimization_barrier(jnp.sum((jnp.cumsum(onehot, axis=1) - onehot) * onehot, axis=-1))
    slot_index = flattened * (N_EP * CAP) + jnp.arange(N_EP, dtype=jnp.int32)[:, None] * CAP + order_rank
    slot_index = slot_index.reshape(-1).astype(jnp.int32)
    repeated = jnp.repeat(ffn_in, TOPK, axis=0)
    buffer = jnp.zeros((EXPERTS * N_EP * CAP, D), jnp.bfloat16).at[slot_index].set(repeated)
    buffer = buffer.reshape(EXPERTS, N_EP * CAP, D)

    def expert(operands):
        rows_in, gate_w, up_w, down_w = operands
        gate_pre = jnp.dot(rows_in, gate_w, preferred_element_type=jnp.float32)
        up_proj = jnp.dot(rows_in, up_w, preferred_element_type=jnp.float32)
        activity = (jax.nn.silu(gate_pre) * up_proj).astype(jnp.bfloat16)
        return jnp.dot(activity, down_w, preferred_element_type=jnp.float32).astype(jnp.bfloat16)
    results = lax.map(expert, (buffer, w_exp_gate, w_exp_up, w_exp_down)).reshape(EXPERTS * N_EP * CAP, D)
    picked = results[slot_index.reshape(BATCH, TOPK)]
    routed = lax.optimization_barrier(jnp.sum(route_weights[..., None] * picked.astype(jnp.float32), axis=1))
    dense_pre = jnp.dot(ffn_in, w_dense_gate.T, preferred_element_type=jnp.float32)
    dense_up = jnp.dot(ffn_in, w_dense_up.T, preferred_element_type=jnp.float32)
    dense_act = (jax.nn.silu(dense_pre) * dense_up).astype(jnp.bfloat16)
    dense_out = jnp.dot(dense_act, w_dense_down, preferred_element_type=jnp.float32)
    dense_gate = jax.nn.sigmoid(lax.optimization_barrier(jnp.sum(ffn_in.astype(jnp.float32) * dense_gate_vector, axis=-1)))
    combined = routed + dense_gate[:, None] * dense_out
    output = (residual.astype(jnp.float32) + normalize(combined, out_gain)).astype(jnp.bfloat16)
    return (output, new_latent, new_rope_key)
```

```python
import functools

import jax
import jax.numpy as jnp
import numpy as np
from jax import lax
from jax.experimental import pallas as pl
from jax.experimental.pallas import tpu as pltpu
from jax.sharding import PartitionSpec as P

epsilon = 1e-06
rope_base = 10000.0
negative = -1e30
MESH = pl.DeviceIdType.MESH
f32 = jnp.float32
bf16 = jnp.bfloat16

NAMES = (
    "tokens", "routes", "rweights", "coef_gain", "w_query", "w_latent",
    "w_abk", "w_rope", "lat_gain", "cache", "rope", "post_gain",
    "ffn_gain", "dvec", "weg", "weu", "wed", "wdg",
    "wdu", "wdd", "out_gain", "inverse", "lengths",
)


def norm(values):
    return values * lax.rsqrt(jnp.mean(values * values, axis=-1, keepdims=True) + epsilon)


def dot(a, b):
    return jnp.dot(a, b, preferred_element_type=f32)


def dot_t(a, b):
    return lax.dot_general(a, b, (((1,), (1,)), ((), ())), preferred_element_type=f32)


def swap_halves(v):
    half = v.shape[1] // 2
    return jnp.concatenate([-v[:, half:], v[:, :half]], axis=1)


def silu(u):
    return u / (1.0 + jnp.exp(-u))


def kernel(ep, tp, *refs):
    n = len(NAMES)
    hbm = dict(zip(NAMES, refs[:n]))
    wv_hbm, wo_hbm = refs[n : 2 + n]
    out_ref, lat_ref, key_ref = refs[2 + n : 5 + n]
    scratch = refs[5 + n :]
    v = dict(zip(NAMES, scratch[:n]))
    (
        wv, wo, load_sem, tokbuf, qsend, qbuf, latsend, latbuf, att, coef, coefbuf,
        xown, xbuf, xrows, psend, pbuf,
        a_s, a_r, q_s, q_r, l_s, l_r, w1_s, w1_r, w2_s, w2_r, c_s, c_r, x_s, x_r, p_s, p_r,
    ) = scratch[n:]
    rows, width = v["tokens"].shape
    heads_local, nope, kv = v["w_abk"].shape
    rope_width = v["w_rope"].shape[0]
    span = nope + rope_width
    heads = heads_local * tp
    scaling = span ** (-0.5)
    me_e = lax.axis_index("ep")
    me_t = lax.axis_index("tp")
    core = lax.rem(me_e, 2)
    sibling = me_e + 1 - 2 * core

    loads = {}
    loads["wv"] = pltpu.make_async_copy(wv_hbm, wv.at[0], load_sem.at[n])
    loads["wo"] = pltpu.make_async_copy(wo_hbm, wo.at[0], load_sem.at[n + 1])
    for i, name in enumerate(NAMES):
        loads[name] = pltpu.make_async_copy(hbm[name], v[name], load_sem.at[i])
    first = ("tokens", "wv", "wo", "routes", "rweights")
    for name in first + tuple(name for name in NAMES if name not in first):
        loads[name].start()

    barrier = pltpu.get_barrier_semaphore()
    for k in range(1, tp):
        pl.semaphore_signal(
            barrier, inc=1, device_id={"tp": lax.rem(me_t + k, tp)}, device_id_type=MESH
        )
    for k in range(1, ep):
        pl.semaphore_signal(
            barrier, inc=1, device_id={"ep": lax.rem(me_e + k, ep)}, device_id_type=MESH
        )

    def tables(count, per):
        row = lax.broadcasted_iota(jnp.int32, (count, rope_width), 0) // per
        pos = jnp.zeros((count, rope_width), jnp.int32)
        for s in range(rows):
            pos = jnp.where(row == s, v["lengths"][:, s : s + 1], pos)
        angles = pos.astype(f32) * v["inverse"][...]
        return jnp.cos(angles), jnp.sin(angles)

    loads["tokens"].wait()
    pl.semaphore_wait(barrier, (tp - 1) + (ep - 1))

    def remote(src, dst, ss, rs, where):
        return pltpu.make_async_remote_copy(
            src_ref=src, dst_ref=dst, send_sem=ss, recv_sem=rs, device_id=where,
            device_id_type=MESH,
        )

    back_t = [lax.rem(me_t + tp - k, tp) for k in range(tp)]
    ahead_t = [lax.rem(me_t + k, tp) for k in range(tp)]
    others = range(ep - 1, 0, -1)
    if ep & (ep - 1) == 0:
        flips = [(1 - 2 * lax.rem(me_e // (1 << i), 2)) * (1 << i) for i in range(ep.bit_length() - 1)]
        to_e = [me_e + sum(f for i, f in enumerate(flips) if k >> i & 1) for k in range(ep)]
        slot, back_to = list(range(ep)), to_e
    else:
        to_e = [lax.rem(me_e + k, ep) for k in range(ep)]
        slot = [(ep - k) % ep for k in range(ep)]
        back_to = to_e
    peers = pl.ds(1, ep - 1)

    def all_of(buf, sem):
        return pltpu.make_async_copy(buf.at[peers], buf.at[peers], sem)

    a_copies = [
        remote(v["tokens"], tokbuf.at[k], a_s.at[k], a_r.at[k], {"tp": back_t[k]})
        for k in range(1, tp)
    ]
    for c in a_copies:
        c.start()
    half_h = heads_local // 2
    depth = wo.shape[1]
    quarter = depth // 8
    part = depth // 16

    def pieces(k):
        start = core * (4 * quarter)
        early = pl.ds(pl.multiple_of(start, quarter), 2 * quarter - part)
        late = pl.ds(pl.multiple_of(start + 2 * quarter - part, part), 2 * quarter + part)
        return (
            wv.at[k, pl.ds(core * half_h, half_h)],
            wo.at[k, early],
            wo.at[k, late],
        )

    w1 = [
        [
            remote(src, dst, w1_s.at[k, i], w1_r.at[k, i], {"tp": back_t[k]})
            for i, (src, dst) in enumerate(zip(pieces(0), pieces(k)))
        ]
        for k in range(1, tp)
    ]
    w2 = [
        [
            remote(dst, dst, w2_s.at[k, i], w2_r.at[k, i], {"ep": sibling})
            for i, dst in enumerate(pieces(k))
        ]
        for k in range(1, tp)
    ]
    loads['wv'].wait()
    loads['wo'].wait()
    for group in w1:
        group[0].start()
        group[1].start()
    loads["routes"].wait()
    loads["rweights"].wait()
    lane = lax.broadcasted_iota(jnp.int32, coef.shape, 1)
    total = jnp.zeros(coef.shape, f32)
    routes = v["routes"][...]
    rweights = v["rweights"][...]
    for k in range(routes.shape[1]):
        total = total + jnp.where(routes[:, k : k + 1] == lane, rweights[:, k : k + 1], 0.0)
    coef[...] = total
    for k in others:
        remote(coef, coefbuf.at[slot[k]], c_s, c_r, {"ep": to_e[k]}).start()

    tokens = v["tokens"][...].astype(f32)
    for c in a_copies:
        c.wait_recv()
    everyone = jnp.concatenate(
        [tokens] + [tokbuf[k].astype(f32) for k in range(1, tp)], axis=0
    )
    loads["coef_gain"].wait()
    hidden = (norm(everyone) * v["coef_gain"][...]).astype(bf16)
    loads["w_query"].wait()
    queries = dot(hidden, v["w_query"][...]).astype(bf16).astype(f32)
    loads["w_latent"].wait()
    latent_part = dot(hidden, v["w_latent"][...])
    loads["w_abk"].wait()
    for h in range(heads_local):
        q_h = queries[:, h * span : h * span + nope].astype(bf16)
        ql = dot(q_h, v["w_abk"][h]).astype(bf16).astype(f32)
        qr = queries[:, h * span + nope : (h + 1) * span]
        for k in range(tp):
            for s in range(rows):
                r = k * rows + s
                target = qbuf if k == 0 else qsend
                target[k, s, h : h + 1, 0:kv] = ql[r : r + 1]
                target[k, s, h : h + 1, kv : kv + rope_width] = qr[r : r + 1]
    for k in range(1, tp):
        latsend[k] = latent_part[k * rows : (k + 1) * rows]
    latbuf[me_t] = latent_part[0:rows]
    q_copies = [
        remote(qsend.at[k], qbuf.at[tp - k], q_s.at[k], q_r.at[tp - k], {"tp": ahead_t[k]})
        for k in range(1, tp)
    ]
    l_copies = [
        remote(latsend.at[k], latbuf.at[me_t], l_s.at[k], l_r.at[tp - k], {"tp": ahead_t[k]})
        for k in range(1, tp)
    ]
    for c in q_copies + l_copies:
        c.start()
    for group in w1:
        group[2].start()
    loads["lengths"].wait()
    loads["inverse"].wait()
    cos_q, sin_q = tables(rows * heads, heads)
    cos_k, sin_k = tables(rows, 1)
    loads["w_rope"].wait()
    raw_key = dot_t(hidden, v["w_rope"][...])[0:rows]
    new_key = (raw_key * cos_k + swap_halves(raw_key) * sin_k).astype(bf16)
    key_ref[...] = new_key
    loads["cache"].wait()
    loads["rope"].wait()
    loads["lat_gain"].wait()
    for c in q_copies + l_copies:
        c.wait_recv()
    for i in (0, 1):
        for group, forward in zip(w1, w2):
            group[i].wait_recv()
            forward[i].start()
    latent = jnp.concatenate([latbuf[t] for t in range(tp)], axis=1)
    new_latent = (norm(latent) * v["lat_gain"][...]).astype(bf16)
    lat_ref[...] = new_latent
    lat_f = new_latent.astype(f32)
    key_f = new_key.astype(f32)
    q_all = jnp.concatenate(
        [qbuf[k, s] for s in range(rows) for k in range(tp)], axis=0
    )
    q_lat = q_all[:, 0:kv]
    q_raw = q_all[:, kv : kv + rope_width]
    q_rot = (q_raw * cos_q + swap_halves(q_raw) * sin_q).astype(bf16)
    def spread(block):
        return jnp.concatenate(
            [jnp.broadcast_to(block[s : s + 1], (heads, block.shape[1])) for s in range(rows)],
            axis=0,
        )

    depth_c = v["cache"].shape[1]
    lat_q = spread(lat_f)
    own = (
        jnp.sum(q_lat * lat_q, axis=1, keepdims=True)
        + jnp.sum(q_rot.astype(f32) * spread(key_f), axis=1, keepdims=True)
    ) * scaling
    q_rot = q_rot.astype(f32)
    blocks = [slice(s * heads, (s + 1) * heads) for s in range(rows)]
    scores = jnp.concatenate(
        [
            dot_t(q_lat[b].astype(bf16), v["cache"][s]) + dot(q_rot[b].astype(bf16), v["rope"][s])
            for s, b in enumerate(blocks)
        ],
        axis=0,
    )
    seq = lax.broadcasted_iota(jnp.int32, (rows * heads, 1), 0) // heads
    limit = jnp.zeros((rows * heads, 1), jnp.int32)
    for s in range(rows):
        limit = jnp.where(seq == s, v["lengths"][:, s : s + 1], limit)
    position = lax.broadcasted_iota(jnp.int32, (rows * heads, depth_c), 1)
    scores = jnp.where(position < limit, scores * scaling, negative)
    top = jnp.maximum(jnp.max(scores, axis=1, keepdims=True), own)
    weights = jnp.exp(scores - top)
    own_weight = jnp.exp(own - top)
    share = 1.0 / (jnp.sum(weights, axis=1, keepdims=True) + own_weight)
    attended = jnp.concatenate(
        [dot(weights[b].astype(bf16), v["cache"][s]) for s, b in enumerate(blocks)], axis=0
    )
    attended = (attended + own_weight * lat_q) * share
    for j in range(kv // 128):
        att[j] = attended[:, j * 128 : (j + 1) * 128]
    for group, forward in zip(w1, w2):
        group[2].wait_recv()
        forward[2].start()
    mixed = jnp.zeros((rows, width), f32)
    for k in range(tp):
        if k > 0:
            for c in w2[k - 1]:
                c.wait_recv()
        parts = []
        for h in range(heads_local):
            chosen = pl.ds(k * heads_local + h, rows, stride=heads)
            picked = jnp.concatenate([att[j, chosen, :] for j in range(kv // 128)], axis=1)
            parts.append(dot_t(picked.astype(bf16), wv[k, h]))
        head_out = jnp.concatenate(parts, axis=1).astype(bf16)
        mixed = mixed + dot(head_out, wo[k]).astype(bf16).astype(f32)
    loads["post_gain"].wait()
    loads["ffn_gain"].wait()
    residual = (tokens + norm(mixed) * v["post_gain"][...]).astype(bf16).astype(f32)
    ffn_in = (norm(residual) * v["ffn_gain"][...]).astype(bf16)
    xown[...] = ffn_in
    for k in others:
        remote(xown, xbuf.at[slot[k]], x_s, x_r, {"ep": to_e[k]}).start()
    for name in ("dvec", "weg", "weu", "wed", "wdg", "wdu", "wdd", "out_gain"):
        loads[name].wait()
    lane_own = lax.broadcasted_iota(jnp.int32, (ep * rows, coef.shape[1]), 1) == me_e

    def own_weight_of(block):
        return jnp.sum(jnp.where(lane_own, block, 0.0), axis=1, keepdims=True)

    all_of(coefbuf, c_r).wait()
    route_w = own_weight_of(
        jnp.concatenate([coef[...]] + [coefbuf[k] for k in range(1, ep)], axis=0)
    )
    xrows[0:rows] = ffn_in.astype(f32)
    all_of(xbuf, x_r).wait()
    for k in range(1, ep):
        xrows[k * rows : (k + 1) * rows] = xbuf[k].astype(f32)
    x_f = xrows[...]
    gate_of = 1.0 / (1.0 + jnp.exp(-jnp.sum(x_f * v["dvec"][...], axis=1, keepdims=True)))
    x = x_f.astype(bf16)
    act_e = (silu(dot(x, v["weg"][0])) * dot(x, v["weu"][0])).astype(bf16)
    act_d = (silu(dot_t(x, v["wdg"][...])) * dot_t(x, v["wdu"][...])).astype(bf16)
    partial = route_w * dot(act_e, v["wed"][0]).astype(bf16).astype(f32) + gate_of * dot(
        act_d, v["wdd"][...]
    )
    for k in range(1, ep):
        psend[k] = partial[k * rows : (k + 1) * rows].astype(bf16)
    for k in others:
        remote(psend.at[k], pbuf.at[k], p_s, p_r, {"ep": back_to[k]}).start()
    combined = partial[0:rows]
    all_of(pbuf, p_r).wait()
    for k in range(1, ep):
        combined = combined + pbuf[k].astype(f32)
    out_ref[...] = (residual + norm(combined) * v["out_gain"][...]).astype(bf16)
    for c in a_copies + q_copies + l_copies:
        c.wait_send()
    for group in w1 + w2:
        for c in group:
            c.wait_send()
    all_of(coefbuf, c_s).wait()
    all_of(xbuf, x_s).wait()
    all_of(psend, p_s).wait()


def hand_over(*refs):
    half = len(refs) // 2
    for src, dst in zip(refs[:half], refs[half:]):
        dst[...] = src[...]


def shards(
    tokens, lengths, cache_latent, cache_rope, attn_gain, latent_gain, post_gain, ffn_gain,
    out_gain, w_latent, w_rope_key, w_query, w_absorb_key, w_absorb_value, w_out, routes,
    route_weights, w_exp_gate, w_exp_up, w_exp_down, w_dense_gate, w_dense_up, w_dense_down,
    dense_gate_vector,
):
    ep, tp = lax.axis_size("ep"), lax.axis_size("tp")
    rows, width = tokens.shape
    heads_local, _, kv = w_absorb_key.shape
    rope_width = w_rope_key.shape[1]
    half = rope_width // 2
    inverse = rope_base ** (-(np.arange(rope_width) % half) / half)
    inverse = jnp.asarray(inverse.reshape(1, -1), f32)

    w_value = jnp.swapaxes(w_absorb_value, 1, 2)

    def flat(g):
        return g.reshape(1, -1)

    ops = [
        tokens, routes, route_weights, flat(attn_gain), w_query, w_latent, w_absorb_key,
        w_rope_key.T, flat(latent_gain), cache_latent, cache_rope, flat(post_gain), flat(ffn_gain),
        flat(dense_gate_vector), w_exp_gate, w_exp_up, w_exp_down, w_dense_gate, w_dense_up,
        w_dense_down, flat(out_gain), inverse, flat(lengths),
    ]
    lanes = -(-ep // 128) * 128
    dma = pltpu.SemaphoreType.DMA
    scratch = [pltpu.VMEM(a.shape, a.dtype) for a in ops]
    scratch += [
        pltpu.VMEM((tp,) + w_value.shape, bf16),
        pltpu.VMEM((tp,) + w_out.shape, bf16),
        dma((len(ops) + 2,)),
        pltpu.VMEM((tp, rows, width), bf16),
        pltpu.VMEM((tp, rows, heads_local, kv + rope_width), f32),
        pltpu.VMEM((tp, rows, heads_local, kv + rope_width), f32),
        pltpu.VMEM((tp, rows, w_latent.shape[1]), f32),
        pltpu.VMEM((tp, rows, w_latent.shape[1]), f32),
        pltpu.VMEM((kv // 128, rows * heads_local * tp, 128), f32),
        pltpu.VMEM((rows, lanes), f32),
        pltpu.VMEM((ep, rows, lanes), f32),
        pltpu.VMEM((rows, width), bf16),
        pltpu.VMEM((ep, rows, width), bf16),
        pltpu.VMEM((ep * rows, width), f32),
        pltpu.VMEM((ep, rows, width), bf16),
        pltpu.VMEM((ep, rows, width), bf16),
    ]
    scratch += [dma((tp,))] * 6 + [dma((tp, 3))] * 4 + [dma] * 6
    anywhere = pl.BlockSpec(memory_space=pl.ANY)
    shapes = (
        jax.ShapeDtypeStruct((rows, width), bf16),
        jax.ShapeDtypeStruct((rows, kv), bf16),
        jax.ShapeDtypeStruct((rows, rope_width), bf16),
    )
    in_vmem = (pl.BlockSpec(memory_space=pltpu.VMEM),) * 3
    results = pl.pallas_call(
        functools.partial(kernel, ep, tp),
        out_shape=shapes,
        in_specs=[anywhere] * (len(ops) + 2),
        out_specs=in_vmem,
        scratch_shapes=scratch,
        compiler_params=pltpu.CompilerParams(
            collective_id=0, has_side_effects=True, vmem_limit_bytes=60 * 1024 * 1024
        ),
    )(*ops, w_value, w_out)
    return tuple(
        pl.pallas_call(hand_over, out_shape=shapes, in_specs=in_vmem, out_specs=in_vmem)(*results)
    )


def solution(mesh):
    placed = (
        P(("ep", "tp"), None),
        P(("ep", "tp")),
        P(("ep", "tp"), None, None),
        P(("ep", "tp"), None, None),
        P(),
        P(),
        P(),
        P(),
        P(),
        P(None, "tp"),
        P(),
        P(None, "tp"),
        P("tp", None, None),
        P("tp", None, None),
        P("tp", None),
        P(("ep", "tp"), None),
        P(("ep", "tp"), None),
        P("ep", None, None),
        P("ep", None, None),
        P("ep", None, None),
        P("ep", None),
        P("ep", None),
        P("ep", None),
        P(),
    )
    return jax.shard_map(
        shards,
        mesh=mesh,
        in_specs=placed,
        out_specs=(P(("ep", "tp"), None), P(("ep", "tp"), None), P(("ep", "tp"), None)),
        check_vma=False,
    )
```

```python
import functools

import jax
import jax.numpy as jnp
import numpy as np
from jax import lax
from jax.experimental import pallas as pl
from jax.experimental.pallas import tpu as pltpu
from jax.sharding import PartitionSpec as P

epsilon = 1e-06
rope_base = 10000.0
negative = -1e30
MESH = pl.DeviceIdType.MESH
f32 = jnp.float32
bf16 = jnp.bfloat16

NAMES = (
    "tokens", "routes", "rweights", "coef_gain", "w_query", "w_latent",
    "w_abk", "w_rope", "lat_gain", "cache", "rope", "post_gain",
    "ffn_gain", "dvec", "weg", "weu", "wed", "wdg",
    "wdu", "wdd", "out_gain", "inverse", "lengths",
)


def norm(values):
    return values * lax.rsqrt(jnp.mean(values * values, axis=-1, keepdims=True) + epsilon)


def dot(a, b):
    return jnp.dot(a, b, preferred_element_type=f32)


def dot_t(a, b):
    return lax.dot_general(a, b, (((1,), (1,)), ((), ())), preferred_element_type=f32)


def swap_halves(v):
    half = v.shape[1] // 2
    return jnp.concatenate([-v[:, half:], v[:, :half]], axis=1)


def silu(u):
    return u / (1.0 + jnp.exp(-u))


def kernel(ep, tp, *refs):
    n = len(NAMES)
    hbm = dict(zip(NAMES, refs[:n]))
    wv_hbm, wo_hbm = refs[n : 2 + n]
    out_ref, lat_ref, key_ref = refs[2 + n : 5 + n]
    scratch = refs[5 + n :]
    v = dict(zip(NAMES, scratch[:n]))
    (
        wv, wo, load_sem, tokbuf, qsend, qbuf, latsend, latbuf, att, coef, coefbuf,
        xown, xbuf, xrows, psend, pbuf,
        a_s, a_r, q_s, q_r, l_s, l_r, wv_sem, wx_s, wf_s, wx_r, wf_r, c_s, c_r, x_s, x_r, p_s, p_r,
    ) = scratch[n:]
    rows, width = v["tokens"].shape
    heads_local, nope, kv = v["w_abk"].shape
    rope_width = v["w_rope"].shape[0]
    span = nope + rope_width
    heads = heads_local * tp
    scaling = span ** (-0.5)
    me_e = lax.axis_index("ep")
    me_t = lax.axis_index("tp")
    core = lax.rem(me_e, 2)
    sibling = me_e + 1 - 2 * core

    loads = {}
    loads["wv"] = pltpu.make_async_copy(wv_hbm, wv.at[0], load_sem.at[n])
    loads["wo"] = pltpu.make_async_copy(wo_hbm, wo.at[0], load_sem.at[n + 1])
    for i, name in enumerate(NAMES):
        loads[name] = pltpu.make_async_copy(hbm[name], v[name], load_sem.at[i])
    first = ("tokens", "wv", "wo", "routes", "rweights")
    for name in first + tuple(name for name in NAMES if name not in first):
        loads[name].start()

    barrier = pltpu.get_barrier_semaphore()
    for k in range(1, tp):
        pl.semaphore_signal(
            barrier, inc=1, device_id={"tp": lax.rem(me_t + k, tp)}, device_id_type=MESH
        )
        pl.semaphore_signal(
            barrier, inc=1, device_id={"tp": lax.rem(me_t + k, tp), "ep": sibling}, device_id_type=MESH
        )
    for k in range(1, ep):
        pl.semaphore_signal(
            barrier, inc=1, device_id={"ep": lax.rem(me_e + k, ep)}, device_id_type=MESH
        )

    def tables(count, per):
        row = lax.broadcasted_iota(jnp.int32, (count, rope_width), 0) // per
        pos = jnp.zeros((count, rope_width), jnp.int32)
        for s in range(rows):
            pos = jnp.where(row == s, v["lengths"][:, s : s + 1], pos)
        angles = pos.astype(f32) * v["inverse"][...]
        return jnp.cos(angles), jnp.sin(angles)

    loads["tokens"].wait()
    pl.semaphore_wait(barrier, 2 * (tp - 1) + (ep - 1))

    def remote(src, dst, ss, rs, where):
        return pltpu.make_async_remote_copy(
            src_ref=src, dst_ref=dst, send_sem=ss, recv_sem=rs, device_id=where,
            device_id_type=MESH,
        )

    back_t = [lax.rem(me_t + tp - k, tp) for k in range(tp)]
    ahead_t = [lax.rem(me_t + k, tp) for k in range(tp)]
    others = range(ep - 1, 0, -1)
    if ep & (ep - 1) == 0:
        flips = [(1 - 2 * lax.rem(me_e // (1 << i), 2)) * (1 << i) for i in range(ep.bit_length() - 1)]
        to_e = [me_e + sum(f for i, f in enumerate(flips) if k >> i & 1) for k in range(ep)]
        slot, back_to = list(range(ep)), to_e
    else:
        to_e = [lax.rem(me_e + k, ep) for k in range(ep)]
        slot = [(ep - k) % ep for k in range(ep)]
        back_to = to_e
    peers = pl.ds(1, ep - 1)

    def all_of(buf, sem):
        return pltpu.make_async_copy(buf.at[peers], buf.at[peers], sem)

    a_copies = [
        remote(v["tokens"], tokbuf.at[k], a_s.at[k], a_r.at[k], {"tp": back_t[k], "ep": sibling})
        for k in range(1, tp)
    ]
    for c in a_copies:
        c.start()
    half_h = heads_local // 2
    depth = wo.shape[1]
    eighth = depth // 8
    step = max(16, eighth // 2)
    member = lax.rem(me_e, 4)

    def wo_rows(k, start, size):
        return wo.at[k, pl.ds(pl.multiple_of(start, 16), size)]

    shared = [(member * eighth + i, step) for i in range(0, eighth, step)]
    local = [
        (depth // 2 + core * (2 * eighth) + i, size)
        for i, size in ((0, eighth), (eighth, step)) + (((eighth + step, step),) if step < eighth else ())
    ]
    n_s, n_l = len(shared), len(local)
    halves = pl.ds(core * half_h, half_h)
    to_mate = {
        j: me_e + sum((1 - 2 * lax.rem(me_e // (1 << i), 2)) * (1 << i) for i in range(2) if j >> i & 1)
        for j in (1, 2, 3)
    }
    x_wv, x_sh, x_lo, f_wv, f_sh, f_lo = [], [], [], [], [], []
    for k in range(1, tp):
        away = {"tp": back_t[k]}
        mine = wv.at[k, halves]
        x_wv.append(remote(wv.at[0, halves], mine, wv_sem.at[0], wv_sem.at[k], away))
        f_wv.append(remote(mine, mine, wv_sem.at[tp], wv_sem.at[tp + k], {"ep": sibling}))
        x_sh.append(
            [
                remote(wo_rows(0, *r), wo_rows(k, *r), wx_s.at[k], wx_r.at[k, i], away)
                for i, r in enumerate(shared)
            ]
        )
        x_lo.append(
            [
                remote(wo_rows(0, *r), wo_rows(k, *r), wx_s.at[k], wx_r.at[k, n_s + i], away)
                for i, r in enumerate(local)
            ]
        )
        f_sh.append(
            [
                [
                    remote(wo_rows(k, *r), wo_rows(k, *r), wf_s.at[k], wf_r.at[k, 3 * i + j - 1], {"ep": to_mate[j]})
                    for j in (2, 3, 1)
                ]
                for i, r in enumerate(shared)
            ]
        )
        f_lo.append(
            [
                remote(wo_rows(k, *r), wo_rows(k, *r), wf_s.at[k], wf_r.at[k, 3 * n_s + i], {"ep": sibling})
                for i, r in enumerate(local)
            ]
        )
    loads["wo"].wait()
    for k in range(tp - 1):
        for c in x_sh[k]:
            c.start()
    loads["wv"].wait()
    for k in range(tp - 1):
        x_wv[k].start()
        x_lo[k][0].start()
    loads["routes"].wait()
    loads["rweights"].wait()
    lane = lax.broadcasted_iota(jnp.int32, coef.shape, 1)
    total = jnp.zeros(coef.shape, f32)
    routes = v["routes"][...]
    rweights = v["rweights"][...]
    for k in range(routes.shape[1]):
        total = total + jnp.where(routes[:, k : k + 1] == lane, rweights[:, k : k + 1], 0.0)
    coef[...] = total
    for k in others:
        remote(coef, coefbuf.at[slot[k]], c_s, c_r, {"ep": to_e[k]}).start()

    tokens = v["tokens"][...].astype(f32)
    for c in a_copies:
        c.wait_recv()
    everyone = jnp.concatenate(
        [tokens] + [tokbuf[k].astype(f32) for k in range(1, tp)], axis=0
    )
    loads["coef_gain"].wait()
    hidden = (norm(everyone) * v["coef_gain"][...]).astype(bf16)
    loads["w_query"].wait()
    queries = dot(hidden, v["w_query"][...]).astype(bf16).astype(f32)
    loads["w_latent"].wait()
    latent_part = dot(hidden, v["w_latent"][...])
    loads["w_abk"].wait()
    for h in range(heads_local):
        q_h = queries[:, h * span : h * span + nope].astype(bf16)
        ql = dot(q_h, v["w_abk"][h]).astype(bf16).astype(f32)
        qr = queries[:, h * span + nope : (h + 1) * span]
        for k in range(tp):
            for s in range(rows):
                r = k * rows + s
                target = qbuf if k == 0 else qsend
                target[k, s, h : h + 1, 0:kv] = ql[r : r + 1]
                target[k, s, h : h + 1, kv : kv + rope_width] = qr[r : r + 1]
    for k in range(1, tp):
        latsend[k] = latent_part[k * rows : (k + 1) * rows]
    latbuf[me_t] = latent_part[0:rows]
    q_copies = [
        remote(qsend.at[k], qbuf.at[tp - k], q_s.at[k], q_r.at[tp - k], {"tp": ahead_t[k], "ep": sibling})
        for k in range(1, tp)
    ]
    l_copies = [
        remote(latsend.at[k], latbuf.at[me_t], l_s.at[k], l_r.at[tp - k], {"tp": ahead_t[k], "ep": sibling})
        for k in range(1, tp)
    ]
    for c in q_copies + l_copies:
        c.start()
    for k in range(tp - 1):
        for c in x_lo[k][1:]:
            c.start()
    loads["lengths"].wait()
    loads["inverse"].wait()
    cos_q, sin_q = tables(rows * heads, heads)
    cos_k, sin_k = tables(rows, 1)
    loads["w_rope"].wait()
    raw_key = dot_t(hidden, v["w_rope"][...])[0:rows]
    new_key = (raw_key * cos_k + swap_halves(raw_key) * sin_k).astype(bf16)
    key_ref[...] = new_key
    for k in range(tp - 1):
        for c, forward in zip(x_sh[k], f_sh[k]):
            c.wait_recv()
            for f in forward:
                f.start()
    loads["cache"].wait()
    loads["rope"].wait()
    loads["lat_gain"].wait()
    for c in q_copies + l_copies:
        c.wait_recv()
    for k in range(tp - 1):
        x_wv[k].wait_recv()
        f_wv[k].start()
    latent = jnp.concatenate([latbuf[t] for t in range(tp)], axis=1)
    new_latent = (norm(latent) * v["lat_gain"][...]).astype(bf16)
    lat_ref[...] = new_latent
    lat_f = new_latent.astype(f32)
    key_f = new_key.astype(f32)
    q_all = jnp.concatenate(
        [qbuf[k, s] for s in range(rows) for k in range(tp)], axis=0
    )
    q_lat = q_all[:, 0:kv]
    q_raw = q_all[:, kv : kv + rope_width]
    q_rot = (q_raw * cos_q + swap_halves(q_raw) * sin_q).astype(bf16)
    def spread(block):
        return jnp.concatenate(
            [jnp.broadcast_to(block[s : s + 1], (heads, block.shape[1])) for s in range(rows)],
            axis=0,
        )

    depth_c = v["cache"].shape[1]
    lat_q = spread(lat_f)
    own = (
        jnp.sum(q_lat * lat_q, axis=1, keepdims=True)
        + jnp.sum(q_rot.astype(f32) * spread(key_f), axis=1, keepdims=True)
    ) * scaling
    q_rot = q_rot.astype(f32)
    blocks = [slice(s * heads, (s + 1) * heads) for s in range(rows)]
    scores = jnp.concatenate(
        [
            dot_t(q_lat[b].astype(bf16), v["cache"][s]) + dot(q_rot[b].astype(bf16), v["rope"][s])
            for s, b in enumerate(blocks)
        ],
        axis=0,
    )
    seq = lax.broadcasted_iota(jnp.int32, (rows * heads, 1), 0) // heads
    limit = jnp.zeros((rows * heads, 1), jnp.int32)
    for s in range(rows):
        limit = jnp.where(seq == s, v["lengths"][:, s : s + 1], limit)
    position = lax.broadcasted_iota(jnp.int32, (rows * heads, depth_c), 1)
    scores = jnp.where(position < limit, scores * scaling, negative)
    top = jnp.maximum(jnp.max(scores, axis=1, keepdims=True), own)
    weights = jnp.exp(scores - top)
    own_weight = jnp.exp(own - top)
    share = 1.0 / (jnp.sum(weights, axis=1, keepdims=True) + own_weight)
    attended = jnp.concatenate(
        [dot(weights[b].astype(bf16), v["cache"][s]) for s, b in enumerate(blocks)], axis=0
    )
    attended = (attended + own_weight * lat_q) * share
    for j in range(kv // 128):
        att[j] = attended[:, j * 128 : (j + 1) * 128]
    for k in range(tp - 1):
        for c, forward in zip(x_lo[k], f_lo[k]):
            c.wait_recv()
            forward.start()
    outs = []
    for k in range(tp):
        if k > 0:
            f_wv[k - 1].wait_recv()
        parts = []
        for h in range(heads_local):
            chosen = pl.ds(k * heads_local + h, rows, stride=heads)
            picked = jnp.concatenate([att[j, chosen, :] for j in range(kv // 128)], axis=1)
            parts.append(dot_t(picked.astype(bf16), wv[k, h]))
        outs.append(jnp.concatenate(parts, axis=1).astype(bf16))
    mixed = dot(outs[0], wo[0]).astype(bf16).astype(f32)
    for k in range(1, tp):
        for forward in f_sh[k - 1]:
            for f in forward:
                f.wait_recv()
        for f in f_lo[k - 1]:
            f.wait_recv()
        mixed = mixed + dot(outs[k], wo[k]).astype(bf16).astype(f32)
    loads["post_gain"].wait()
    loads["ffn_gain"].wait()
    residual = (tokens + norm(mixed) * v["post_gain"][...]).astype(bf16).astype(f32)
    ffn_in = (norm(residual) * v["ffn_gain"][...]).astype(bf16)
    xown[...] = ffn_in
    for k in others:
        remote(xown, xbuf.at[slot[k]], x_s, x_r, {"ep": to_e[k]}).start()
    for name in ("dvec", "weg", "weu", "wed", "wdg", "wdu", "wdd", "out_gain"):
        loads[name].wait()
    lane_own = lax.broadcasted_iota(jnp.int32, (ep * rows, coef.shape[1]), 1) == me_e

    def own_weight_of(block):
        return jnp.sum(jnp.where(lane_own, block, 0.0), axis=1, keepdims=True)

    all_of(coefbuf, c_r).wait()
    route_w = own_weight_of(
        jnp.concatenate([coef[...]] + [coefbuf[k] for k in range(1, ep)], axis=0)
    )
    xrows[0:rows] = ffn_in.astype(f32)
    all_of(xbuf, x_r).wait()
    for k in range(1, ep):
        xrows[k * rows : (k + 1) * rows] = xbuf[k].astype(f32)
    x_f = xrows[...]
    gate_of = 1.0 / (1.0 + jnp.exp(-jnp.sum(x_f * v["dvec"][...], axis=1, keepdims=True)))
    x = x_f.astype(bf16)
    act_e = (silu(dot(x, v["weg"][0])) * dot(x, v["weu"][0])).astype(bf16)
    act_d = (silu(dot_t(x, v["wdg"][...])) * dot_t(x, v["wdu"][...])).astype(bf16)
    partial = route_w * dot(act_e, v["wed"][0]).astype(bf16).astype(f32) + gate_of * dot(
        act_d, v["wdd"][...]
    )
    for k in range(1, ep):
        psend[k] = partial[k * rows : (k + 1) * rows].astype(bf16)
    for k in others:
        remote(psend.at[k], pbuf.at[k], p_s, p_r, {"ep": back_to[k]}).start()
    combined = partial[0:rows]
    all_of(pbuf, p_r).wait()
    for k in range(1, ep):
        combined = combined + pbuf[k].astype(f32)
    out_ref[...] = (residual + norm(combined) * v["out_gain"][...]).astype(bf16)
    for c in a_copies + q_copies + l_copies:
        c.wait_send()
    for k in range(tp - 1):
        pltpu.make_async_copy(
            wo_rows(k + 1, 0, 3 * eighth), wo_rows(k + 1, 0, 3 * eighth), wx_s.at[k + 1]
        ).wait()
        pltpu.make_async_copy(
            wo_rows(k + 1, 0, 5 * eighth), wo_rows(k + 1, 0, 5 * eighth), wf_s.at[k + 1]
        ).wait()
    every = wv.at[pl.ds(1, tp - 1), halves]
    pltpu.make_async_copy(every, every, wv_sem.at[0]).wait()
    pltpu.make_async_copy(every, every, wv_sem.at[tp]).wait()
    all_of(coefbuf, c_s).wait()
    all_of(xbuf, x_s).wait()
    all_of(psend, p_s).wait()


def hand_over(*refs):
    half = len(refs) // 2
    for src, dst in zip(refs[:half], refs[half:]):
        dst[...] = src[...]


def shards(
    tokens, lengths, cache_latent, cache_rope, attn_gain, latent_gain, post_gain, ffn_gain,
    out_gain, w_latent, w_rope_key, w_query, w_absorb_key, w_absorb_value, w_out, routes,
    route_weights, w_exp_gate, w_exp_up, w_exp_down, w_dense_gate, w_dense_up, w_dense_down,
    dense_gate_vector,
):
    ep, tp = lax.axis_size("ep"), lax.axis_size("tp")
    rows, width = tokens.shape
    heads_local, _, kv = w_absorb_key.shape
    rope_width = w_rope_key.shape[1]
    half = rope_width // 2
    inverse = rope_base ** (-(np.arange(rope_width) % half) / half)
    inverse = jnp.asarray(inverse.reshape(1, -1), f32)

    w_value = jnp.swapaxes(w_absorb_value, 1, 2)

    def flat(g):
        return g.reshape(1, -1)

    ops = [
        tokens, routes, route_weights, flat(attn_gain), w_query, w_latent, w_absorb_key,
        w_rope_key.T, flat(latent_gain), cache_latent, cache_rope, flat(post_gain), flat(ffn_gain),
        flat(dense_gate_vector), w_exp_gate, w_exp_up, w_exp_down, w_dense_gate, w_dense_up,
        w_dense_down, flat(out_gain), inverse, flat(lengths),
    ]
    lanes = -(-ep // 128) * 128
    dma = pltpu.SemaphoreType.DMA
    scratch = [pltpu.VMEM(a.shape, a.dtype) for a in ops]
    scratch += [
        pltpu.VMEM((tp,) + w_value.shape, bf16),
        pltpu.VMEM((tp,) + w_out.shape, bf16),
        dma((len(ops) + 2,)),
        pltpu.VMEM((tp, rows, width), bf16),
        pltpu.VMEM((tp, rows, heads_local, kv + rope_width), f32),
        pltpu.VMEM((tp, rows, heads_local, kv + rope_width), f32),
        pltpu.VMEM((tp, rows, w_latent.shape[1]), f32),
        pltpu.VMEM((tp, rows, w_latent.shape[1]), f32),
        pltpu.VMEM((kv // 128, rows * heads_local * tp, 128), f32),
        pltpu.VMEM((rows, lanes), f32),
        pltpu.VMEM((ep, rows, lanes), f32),
        pltpu.VMEM((rows, width), bf16),
        pltpu.VMEM((ep, rows, width), bf16),
        pltpu.VMEM((ep * rows, width), f32),
        pltpu.VMEM((ep, rows, width), bf16),
        pltpu.VMEM((ep, rows, width), bf16),
    ]
    scratch += [dma((tp,))] * 6 + [dma((2 * tp,)), dma((tp,)), dma((tp,)), dma((tp, 5)), dma((tp, 9))]
    scratch += [dma] * 6
    anywhere = pl.BlockSpec(memory_space=pl.ANY)
    shapes = (
        jax.ShapeDtypeStruct((rows, width), bf16),
        jax.ShapeDtypeStruct((rows, kv), bf16),
        jax.ShapeDtypeStruct((rows, rope_width), bf16),
    )
    in_vmem = (pl.BlockSpec(memory_space=pltpu.VMEM),) * 3
    results = pl.pallas_call(
        functools.partial(kernel, ep, tp),
        out_shape=tuple(pltpu.VMEM(o.shape, o.dtype) for o in shapes),
        in_specs=[anywhere] * (len(ops) + 2),
        out_specs=in_vmem,
        scratch_shapes=scratch,
        compiler_params=pltpu.CompilerParams(
            collective_id=0, has_side_effects=True, vmem_limit_bytes=60 * 1024 * 1024
        ),
    )(*ops, w_value, w_out)
    return tuple(
        pl.pallas_call(hand_over, out_shape=shapes, in_specs=in_vmem, out_specs=in_vmem)(*[pltpu.with_memory_space_constraint(r, pltpu.VMEM) for r in results])
    )


def solution(mesh):
    placed = (
        P(("ep", "tp"), None),
        P(("ep", "tp")),
        P(("ep", "tp"), None, None),
        P(("ep", "tp"), None, None),
        P(),
        P(),
        P(),
        P(),
        P(),
        P(None, "tp"),
        P(),
        P(None, "tp"),
        P("tp", None, None),
        P("tp", None, None),
        P("tp", None),
        P(("ep", "tp"), None),
        P(("ep", "tp"), None),
        P("ep", None, None),
        P("ep", None, None),
        P("ep", None, None),
        P("ep", None),
        P("ep", None),
        P("ep", None),
        P(),
    )
    return jax.shard_map(
        shards,
        mesh=mesh,
        in_specs=placed,
        out_specs=(P(("ep", "tp"), None), P(("ep", "tp"), None), P(("ep", "tp"), None)),
        check_vma=False,
    )
```

```python
import functools

import jax
import jax.numpy as jnp
import numpy as np
from jax import lax
from jax.experimental import pallas as pl
from jax.experimental.pallas import tpu as pltpu
from jax.sharding import PartitionSpec as P

epsilon = 1e-06
rope_base = 10000.0
negative = -1e30
MESH = pl.DeviceIdType.MESH
f32 = jnp.float32
bf16 = jnp.bfloat16

NAMES = (
    "tokens", "routes", "rweights", "coef_gain", "w_query", "w_latent",
    "w_abk", "w_rope", "lat_gain", "cache", "rope", "post_gain",
    "ffn_gain", "dvec", "weg", "weu", "wed", "wdg",
    "wdu", "wdd", "out_gain", "inverse", "lengths",
)


def norm(values):
    return values * lax.rsqrt(jnp.mean(values * values, axis=-1, keepdims=True) + epsilon)


def dot(a, b):
    return jnp.dot(a, b, preferred_element_type=f32)


def dot_t(a, b):
    return lax.dot_general(a, b, (((1,), (1,)), ((), ())), preferred_element_type=f32)


def swap_halves(v):
    half = v.shape[1] // 2
    return jnp.concatenate([-v[:, half:], v[:, :half]], axis=1)


def silu(u):
    return u / (1.0 + jnp.exp(-u))


def kernel(ep, tp, *refs):
    n = len(NAMES)
    hbm = dict(zip(NAMES, refs[:n]))
    wv_hbm, wo_hbm = refs[n : 2 + n]
    out_ref, lat_ref, key_ref = refs[2 + n : 5 + n]
    scratch = refs[5 + n :]
    v = dict(zip(NAMES, scratch[:n]))
    (
        wv, wo, load_sem, tokbuf, qsend, qbuf, latsend, latbuf, att, coef, coefbuf,
        xown, xbuf, xrows, psend, pbuf,
        a_s, a_r, q_s, q_r, l_s, l_r, wv_sem, wx_s, wf_s, wx_r, wf_r, known, c_s, c_r, x_s, x_r, p_s, p_r,
    ) = scratch[n:]
    rows, width = v["tokens"].shape
    heads_local, nope, kv = v["w_abk"].shape
    rope_width = v["w_rope"].shape[0]
    span = nope + rope_width
    heads = heads_local * tp
    scaling = span ** (-0.5)
    me_e = lax.axis_index("ep")
    me_t = lax.axis_index("tp")
    core = lax.rem(me_e, 2)
    sibling = me_e + 1 - 2 * core

    loads = {}
    loads["wv"] = pltpu.make_async_copy(wv_hbm, wv.at[0], load_sem.at[n])
    loads["wo"] = pltpu.make_async_copy(wo_hbm, wo.at[0], load_sem.at[n + 1])
    for i, name in enumerate(NAMES):
        loads[name] = pltpu.make_async_copy(hbm[name], v[name], load_sem.at[i])
    first = ("tokens", "wv", "wo", "routes", "rweights")
    for name in first + tuple(name for name in NAMES if name not in first):
        loads[name].start()

    barrier = pltpu.get_barrier_semaphore()
    for k in range(1, tp):
        pl.semaphore_signal(
            barrier, inc=1, device_id={"tp": lax.rem(me_t + k, tp)}, device_id_type=MESH
        )
        pl.semaphore_signal(
            barrier, inc=1, device_id={"tp": lax.rem(me_t + k, tp), "ep": sibling}, device_id_type=MESH
        )
    quads = ep // 4
    quad = me_e // 4

    def mate(j):
        return me_e + sum(
            (1 - 2 * lax.rem(me_e // (1 << i), 2)) * (1 << i) for i in range(2) if j >> i & 1
        )

    def greet(sem, where):
        pl.semaphore_signal(sem, inc=1, device_id=where, device_id_type=MESH)

    def greet_line(sem, reach):
        @pl.when(quad >= reach)
        def _():
            greet(sem, {"ep": me_e - 4 * reach})

        @pl.when(quad < quads - reach)
        def _():
            greet(sem, {"ep": me_e + 4 * reach})

    def in_line(reach):
        return (quad >= reach).astype(jnp.int32) + (quad < quads - reach).astype(jnp.int32)

    def greet_mates(sem):
        for j in (2, 3, 1):
            greet(sem, {"ep": mate(j)})

    stages = (quads - 1).bit_length()
    greet_mates(barrier)
    greet_line(barrier, 1)

    def tables(count, per):
        row = lax.broadcasted_iota(jnp.int32, (count, rope_width), 0) // per
        pos = jnp.zeros((count, rope_width), jnp.int32)
        for s in range(rows):
            pos = jnp.where(row == s, v["lengths"][:, s : s + 1], pos)
        angles = pos.astype(f32) * v["inverse"][...]
        return jnp.cos(angles), jnp.sin(angles)

    loads["tokens"].wait()
    pl.semaphore_wait(barrier, 2 * (tp - 1) + 3 + in_line(1))

    def remote(src, dst, ss, rs, where):
        return pltpu.make_async_remote_copy(
            src_ref=src, dst_ref=dst, send_sem=ss, recv_sem=rs, device_id=where,
            device_id_type=MESH,
        )

    back_t = [lax.rem(me_t + tp - k, tp) for k in range(tp)]
    ahead_t = [lax.rem(me_t + k, tp) for k in range(tp)]
    others = range(ep - 1, 0, -1)
    if ep & (ep - 1) == 0:
        flips = [(1 - 2 * lax.rem(me_e // (1 << i), 2)) * (1 << i) for i in range(ep.bit_length() - 1)]
        to_e = [me_e + sum(f for i, f in enumerate(flips) if k >> i & 1) for k in range(ep)]
        slot, back_to = list(range(ep)), to_e
    else:
        to_e = [lax.rem(me_e + k, ep) for k in range(ep)]
        slot = [(ep - k) % ep for k in range(ep)]
        back_to = to_e
    peers = pl.ds(1, ep - 1)

    def all_of(buf, sem):
        return pltpu.make_async_copy(buf.at[peers], buf.at[peers], sem)

    a_copies = [
        remote(v["tokens"], tokbuf.at[k], a_s.at[k], a_r.at[k], {"tp": back_t[k], "ep": sibling})
        for k in range(1, tp)
    ]
    for c in a_copies:
        c.start()
    greet_line(known.at[0], 1)
    half_h = heads_local // 2
    depth = wo.shape[1]
    eighth = depth // 8
    step = max(16, eighth // 2)
    member = lax.rem(me_e, 4)

    def wo_rows(k, start, size):
        return wo.at[k, pl.ds(pl.multiple_of(start, 16), size)]

    shared = [(member * eighth + i, step) for i in range(0, eighth, step)]
    local = [
        (depth // 2 + core * (2 * eighth) + i, size)
        for i, size in ((0, eighth), (eighth, step)) + (((eighth + step, step),) if step < eighth else ())
    ]
    n_s, n_l = len(shared), len(local)
    halves = pl.ds(core * half_h, half_h)
    x_wv, x_sh, x_lo, f_wv, f_sh, f_lo = [], [], [], [], [], []
    for k in range(1, tp):
        away = {"tp": back_t[k]}
        mine = wv.at[k, halves]
        x_wv.append(remote(wv.at[0, halves], mine, wv_sem.at[0], wv_sem.at[k], away))
        f_wv.append(remote(mine, mine, wv_sem.at[tp], wv_sem.at[tp + k], {"ep": sibling}))
        x_sh.append(
            [
                remote(wo_rows(0, *r), wo_rows(k, *r), wx_s.at[k], wx_r.at[k, i], away)
                for i, r in enumerate(shared)
            ]
        )
        x_lo.append(
            [
                remote(wo_rows(0, *r), wo_rows(k, *r), wx_s.at[k], wx_r.at[k, n_s + i], away)
                for i, r in enumerate(local)
            ]
        )
        f_sh.append(
            [
                [
                    remote(wo_rows(k, *r), wo_rows(k, *r), wf_s.at[k], wf_r.at[k, 3 * i + j - 1], {"ep": mate(j)})
                    for j in (2, 3, 1)
                ]
                for i, r in enumerate(shared)
            ]
        )
        f_lo.append(
            [
                remote(wo_rows(k, *r), wo_rows(k, *r), wf_s.at[k], wf_r.at[k, 3 * n_s + i], {"ep": sibling})
                for i, r in enumerate(local)
            ]
        )
    loads["wo"].wait()
    for k in range(tp - 1):
        for c in x_sh[k]:
            c.start()
    loads["wv"].wait()
    for k in range(tp - 1):
        x_wv[k].start()
        x_lo[k][0].start()
    loads["routes"].wait()
    loads["rweights"].wait()
    lane = lax.broadcasted_iota(jnp.int32, coef.shape, 1)
    total = jnp.zeros(coef.shape, f32)
    routes = v["routes"][...]
    rweights = v["rweights"][...]
    for k in range(routes.shape[1]):
        total = total + jnp.where(routes[:, k : k + 1] == lane, rweights[:, k : k + 1], 0.0)
    coef[...] = total
    tokens = v["tokens"][...].astype(f32)
    for c in a_copies:
        c.wait_recv()
    everyone = jnp.concatenate(
        [tokens] + [tokbuf[k].astype(f32) for k in range(1, tp)], axis=0
    )
    loads["coef_gain"].wait()
    hidden = (norm(everyone) * v["coef_gain"][...]).astype(bf16)
    loads["w_query"].wait()
    queries = dot(hidden, v["w_query"][...]).astype(bf16).astype(f32)
    loads["w_latent"].wait()
    latent_part = dot(hidden, v["w_latent"][...])
    loads["w_abk"].wait()
    for h in range(heads_local):
        q_h = queries[:, h * span : h * span + nope].astype(bf16)
        ql = dot(q_h, v["w_abk"][h]).astype(bf16).astype(f32)
        qr = queries[:, h * span + nope : (h + 1) * span]
        for k in range(tp):
            for s in range(rows):
                r = k * rows + s
                target = qbuf if k == 0 else qsend
                target[k, s, h : h + 1, 0:kv] = ql[r : r + 1]
                target[k, s, h : h + 1, kv : kv + rope_width] = qr[r : r + 1]
    for k in range(1, tp):
        latsend[k] = latent_part[k * rows : (k + 1) * rows]
    latbuf[me_t] = latent_part[0:rows]
    q_copies = [
        remote(qsend.at[k], qbuf.at[tp - k], q_s.at[k], q_r.at[tp - k], {"tp": ahead_t[k], "ep": sibling})
        for k in range(1, tp)
    ]
    l_copies = [
        remote(latsend.at[k], latbuf.at[me_t], l_s.at[k], l_r.at[tp - k], {"tp": ahead_t[k], "ep": sibling})
        for k in range(1, tp)
    ]
    for c in q_copies + l_copies:
        c.start()
    for k in range(tp - 1):
        for c in x_lo[k][1:]:
            c.start()
    pl.semaphore_wait(known.at[0], in_line(1))
    if stages > 1:
        greet_line(known.at[1], 2)
    loads["lengths"].wait()
    loads["inverse"].wait()
    cos_q, sin_q = tables(rows * heads, heads)
    cos_k, sin_k = tables(rows, 1)
    loads["w_rope"].wait()
    raw_key = dot_t(hidden, v["w_rope"][...])[0:rows]
    new_key = (raw_key * cos_k + swap_halves(raw_key) * sin_k).astype(bf16)
    key_ref[...] = new_key
    for k in range(tp - 1):
        for c, forward in zip(x_sh[k], f_sh[k]):
            c.wait_recv()
            for f in forward:
                f.start()
    loads["cache"].wait()
    loads["rope"].wait()
    loads["lat_gain"].wait()
    for c in q_copies + l_copies:
        c.wait_recv()
    for k in range(tp - 1):
        x_wv[k].wait_recv()
        f_wv[k].start()
    for stage in range(1, stages):
        pl.semaphore_wait(known.at[stage], in_line(1 << stage))
        if stage + 1 < stages:
            greet_line(known.at[stage + 1], 2 << stage)
    greet_mates(known.at[stages])
    latent = jnp.concatenate([latbuf[t] for t in range(tp)], axis=1)
    new_latent = (norm(latent) * v["lat_gain"][...]).astype(bf16)
    lat_ref[...] = new_latent
    lat_f = new_latent.astype(f32)
    key_f = new_key.astype(f32)
    q_all = jnp.concatenate(
        [qbuf[k, s] for s in range(rows) for k in range(tp)], axis=0
    )
    q_lat = q_all[:, 0:kv]
    q_raw = q_all[:, kv : kv + rope_width]
    q_rot = (q_raw * cos_q + swap_halves(q_raw) * sin_q).astype(bf16)
    def spread(block):
        return jnp.concatenate(
            [jnp.broadcast_to(block[s : s + 1], (heads, block.shape[1])) for s in range(rows)],
            axis=0,
        )

    depth_c = v["cache"].shape[1]
    lat_q = spread(lat_f)
    own = (
        jnp.sum(q_lat * lat_q, axis=1, keepdims=True)
        + jnp.sum(q_rot.astype(f32) * spread(key_f), axis=1, keepdims=True)
    ) * scaling
    q_rot = q_rot.astype(f32)
    blocks = [slice(s * heads, (s + 1) * heads) for s in range(rows)]
    scores = jnp.concatenate(
        [
            dot_t(q_lat[b].astype(bf16), v["cache"][s]) + dot(q_rot[b].astype(bf16), v["rope"][s])
            for s, b in enumerate(blocks)
        ],
        axis=0,
    )
    seq = lax.broadcasted_iota(jnp.int32, (rows * heads, 1), 0) // heads
    limit = jnp.zeros((rows * heads, 1), jnp.int32)
    for s in range(rows):
        limit = jnp.where(seq == s, v["lengths"][:, s : s + 1], limit)
    position = lax.broadcasted_iota(jnp.int32, (rows * heads, depth_c), 1)
    scores = jnp.where(position < limit, scores * scaling, negative)
    top = jnp.maximum(jnp.max(scores, axis=1, keepdims=True), own)
    weights = jnp.exp(scores - top)
    own_weight = jnp.exp(own - top)
    share = 1.0 / (jnp.sum(weights, axis=1, keepdims=True) + own_weight)
    attended = jnp.concatenate(
        [dot(weights[b].astype(bf16), v["cache"][s]) for s, b in enumerate(blocks)], axis=0
    )
    attended = (attended + own_weight * lat_q) * share
    for j in range(kv // 128):
        att[j] = attended[:, j * 128 : (j + 1) * 128]
    pl.semaphore_wait(known.at[stages], 3)
    for k in others:
        remote(coef, coefbuf.at[slot[k]], c_s, c_r, {"ep": to_e[k]}).start()
    for k in range(tp - 1):
        for c, forward in zip(x_lo[k], f_lo[k]):
            c.wait_recv()
            forward.start()
    outs = []
    for k in range(tp):
        if k > 0:
            f_wv[k - 1].wait_recv()
        parts = []
        for h in range(heads_local):
            chosen = pl.ds(k * heads_local + h, rows, stride=heads)
            picked = jnp.concatenate([att[j, chosen, :] for j in range(kv // 128)], axis=1)
            parts.append(dot_t(picked.astype(bf16), wv[k, h]))
        outs.append(jnp.concatenate(parts, axis=1).astype(bf16))
    mixed = dot(outs[0], wo[0]).astype(bf16).astype(f32)
    for k in range(1, tp):
        for forward in f_sh[k - 1]:
            for f in forward:
                f.wait_recv()
        for f in f_lo[k - 1]:
            f.wait_recv()
        mixed = mixed + dot(outs[k], wo[k]).astype(bf16).astype(f32)
    loads["post_gain"].wait()
    loads["ffn_gain"].wait()
    residual = (tokens + norm(mixed) * v["post_gain"][...]).astype(bf16).astype(f32)
    ffn_in = (norm(residual) * v["ffn_gain"][...]).astype(bf16)
    xown[...] = ffn_in
    for k in others:
        remote(xown, xbuf.at[slot[k]], x_s, x_r, {"ep": to_e[k]}).start()
    for name in ("dvec", "weg", "weu", "wed", "wdg", "wdu", "wdd", "out_gain"):
        loads[name].wait()
    lane_own = lax.broadcasted_iota(jnp.int32, (ep * rows, coef.shape[1]), 1) == me_e

    def own_weight_of(block):
        return jnp.sum(jnp.where(lane_own, block, 0.0), axis=1, keepdims=True)

    all_of(coefbuf, c_r).wait()
    route_w = own_weight_of(
        jnp.concatenate([coef[...]] + [coefbuf[k] for k in range(1, ep)], axis=0)
    )
    xrows[0:rows] = ffn_in.astype(f32)
    all_of(xbuf, x_r).wait()
    for k in range(1, ep):
        xrows[k * rows : (k + 1) * rows] = xbuf[k].astype(f32)
    x_f = xrows[...]
    gate_of = 1.0 / (1.0 + jnp.exp(-jnp.sum(x_f * v["dvec"][...], axis=1, keepdims=True)))
    x = x_f.astype(bf16)
    act_e = (silu(dot(x, v["weg"][0])) * dot(x, v["weu"][0])).astype(bf16)
    act_d = (silu(dot_t(x, v["wdg"][...])) * dot_t(x, v["wdu"][...])).astype(bf16)
    partial = route_w * dot(act_e, v["wed"][0]).astype(bf16).astype(f32) + gate_of * dot(
        act_d, v["wdd"][...]
    )
    for k in range(1, ep):
        psend[k] = partial[k * rows : (k + 1) * rows].astype(bf16)
    for k in others:
        remote(psend.at[k], pbuf.at[k], p_s, p_r, {"ep": back_to[k]}).start()
    combined = partial[0:rows]
    all_of(pbuf, p_r).wait()
    for k in range(1, ep):
        combined = combined + pbuf[k].astype(f32)
    out_ref[...] = (residual + norm(combined) * v["out_gain"][...]).astype(bf16)
    for c in a_copies + q_copies + l_copies:
        c.wait_send()
    for k in range(tp - 1):
        pltpu.make_async_copy(
            wo_rows(k + 1, 0, 3 * eighth), wo_rows(k + 1, 0, 3 * eighth), wx_s.at[k + 1]
        ).wait()
        pltpu.make_async_copy(
            wo_rows(k + 1, 0, 5 * eighth), wo_rows(k + 1, 0, 5 * eighth), wf_s.at[k + 1]
        ).wait()
    every = wv.at[pl.ds(1, tp - 1), halves]
    pltpu.make_async_copy(every, every, wv_sem.at[0]).wait()
    pltpu.make_async_copy(every, every, wv_sem.at[tp]).wait()
    all_of(coefbuf, c_s).wait()
    all_of(xbuf, x_s).wait()
    all_of(psend, p_s).wait()


def hand_over(*refs):
    half = len(refs) // 2
    for src, dst in zip(refs[:half], refs[half:]):
        dst[...] = src[...]


def shards(
    tokens, lengths, cache_latent, cache_rope, attn_gain, latent_gain, post_gain, ffn_gain,
    out_gain, w_latent, w_rope_key, w_query, w_absorb_key, w_absorb_value, w_out, routes,
    route_weights, w_exp_gate, w_exp_up, w_exp_down, w_dense_gate, w_dense_up, w_dense_down,
    dense_gate_vector,
):
    ep, tp = lax.axis_size("ep"), lax.axis_size("tp")
    rows, width = tokens.shape
    heads_local, _, kv = w_absorb_key.shape
    rope_width = w_rope_key.shape[1]
    half = rope_width // 2
    inverse = rope_base ** (-(np.arange(rope_width) % half) / half)
    inverse = jnp.asarray(inverse.reshape(1, -1), f32)

    w_value = jnp.swapaxes(w_absorb_value, 1, 2)

    def flat(g):
        return g.reshape(1, -1)

    ops = [
        tokens, routes, route_weights, flat(attn_gain), w_query, w_latent, w_absorb_key,
        w_rope_key.T, flat(latent_gain), cache_latent, cache_rope, flat(post_gain), flat(ffn_gain),
        flat(dense_gate_vector), w_exp_gate, w_exp_up, w_exp_down, w_dense_gate, w_dense_up,
        w_dense_down, flat(out_gain), inverse, flat(lengths),
    ]
    lanes = -(-ep // 128) * 128
    dma = pltpu.SemaphoreType.DMA
    scratch = [pltpu.VMEM(a.shape, a.dtype) for a in ops]
    scratch += [
        pltpu.VMEM((tp,) + w_value.shape, bf16),
        pltpu.VMEM((tp,) + w_out.shape, bf16),
        dma((len(ops) + 2,)),
        pltpu.VMEM((tp, rows, width), bf16),
        pltpu.VMEM((tp, rows, heads_local, kv + rope_width), f32),
        pltpu.VMEM((tp, rows, heads_local, kv + rope_width), f32),
        pltpu.VMEM((tp, rows, w_latent.shape[1]), f32),
        pltpu.VMEM((tp, rows, w_latent.shape[1]), f32),
        pltpu.VMEM((kv // 128, rows * heads_local * tp, 128), f32),
        pltpu.VMEM((rows, lanes), f32),
        pltpu.VMEM((ep, rows, lanes), f32),
        pltpu.VMEM((rows, width), bf16),
        pltpu.VMEM((ep, rows, width), bf16),
        pltpu.VMEM((ep * rows, width), f32),
        pltpu.VMEM((ep, rows, width), bf16),
        pltpu.VMEM((ep, rows, width), bf16),
    ]
    scratch += [dma((tp,))] * 6 + [dma((2 * tp,)), dma((tp,)), dma((tp,)), dma((tp, 5)), dma((tp, 9))]
    scratch += [pltpu.SemaphoreType.REGULAR(((ep // 4 - 1).bit_length() + 1,))]
    scratch += [dma] * 6
    anywhere = pl.BlockSpec(memory_space=pl.ANY)
    shapes = (
        jax.ShapeDtypeStruct((rows, width), bf16),
        jax.ShapeDtypeStruct((rows, kv), bf16),
        jax.ShapeDtypeStruct((rows, rope_width), bf16),
    )
    in_vmem = (pl.BlockSpec(memory_space=pltpu.VMEM),) * 3
    results = pl.pallas_call(
        functools.partial(kernel, ep, tp),
        out_shape=tuple(pltpu.VMEM(o.shape, o.dtype) for o in shapes),
        in_specs=[anywhere] * (len(ops) + 2),
        out_specs=in_vmem,
        scratch_shapes=scratch,
        compiler_params=pltpu.CompilerParams(
            collective_id=0, has_side_effects=True, vmem_limit_bytes=60 * 1024 * 1024
        ),
    )(*ops, w_value, w_out)
    return tuple(
        pl.pallas_call(hand_over, out_shape=shapes, in_specs=in_vmem, out_specs=in_vmem)(*[pltpu.with_memory_space_constraint(r, pltpu.VMEM) for r in results])
    )


def solution(mesh):
    placed = (
        P(("ep", "tp"), None),
        P(("ep", "tp")),
        P(("ep", "tp"), None, None),
        P(("ep", "tp"), None, None),
        P(),
        P(),
        P(),
        P(),
        P(),
        P(None, "tp"),
        P(),
        P(None, "tp"),
        P("tp", None, None),
        P("tp", None, None),
        P("tp", None),
        P(("ep", "tp"), None),
        P(("ep", "tp"), None),
        P("ep", None, None),
        P("ep", None, None),
        P("ep", None, None),
        P("ep", None),
        P("ep", None),
        P("ep", None),
        P(),
    )
    return jax.shard_map(
        shards,
        mesh=mesh,
        in_specs=placed,
        out_specs=(P(("ep", "tp"), None), P(("ep", "tp"), None), P(("ep", "tp"), None)),
        check_vma=False,
    )
```
